32 devices in a mesh: ep: 16 (over z, x, core), tp: 2 (over y).
Axes of the slice: x: 2, y: 2, z: 4, core: 2. Of those that a mesh axis runs over, the one named last changes fastest.
Arguments:
- tokens: bfloat16 [2048, 2048], P('ep'), may hold values from -6 to 6
- routes: int32 [2048, 2], P('ep'), may hold values from 0 to 3, all different within a row; in each aligned block of 128 rows (0 to 127, 128 to 255, ...) at most 80 rows name the same one
- router_weight: bfloat16 [2048, 4], replicated, may hold values from -0.125 to 0.125
- gate_proj: bfloat16 [16, 2048, 1024], P('ep', None, 'tp'), may hold values from -0.125 to 0.125
- up_proj: bfloat16 [16, 2048, 1024], P('ep', None, 'tp'), may hold values from -0.125 to 0.125
- down_proj: bfloat16 [16, 1024, 2048], P('ep', 'tp'), may hold values from -0.09375 to 0.09375
- cotangent: bfloat16 [2048, 2048], P('ep'), may hold values from -1.5 to 1.5
Outputs:
- token_grad: bfloat16 [2048, 2048], P('ep', 'tp')
- gate_grad: float32 [2048, 2], P('ep')
- router_grad: float32 [2048, 4], P('ep')
- gate_proj_grad: float32 [16, 2048, 1024], P('ep', None, 'tp')
- up_proj_grad: float32 [16, 2048, 1024], P('ep', None, 'tp')
- down_proj_grad: float32 [16, 1024, 2048], P('ep', 'tp')
The draws below stay inside these ranges and needn't reach their ends.
Inputs may be any that keep to these rules, and one draw needn't show every extreme that they name: `routes`: each row names 2 different experts. Among the rows of one index of ep no expert is named more than 80 times, a bound that some block reaches.
All inputs are finite; a program needn't handle non-finite values.
Results may differ from the reference program's by a relative error of at most 0.0085.
Values may be sent and summed in bfloat16 or wider, within the bound.
No kernel may reach another device: no remote copies, remote signals or barrier semaphores. Data moves between devices by JAX's collectives and lax.ppermute only.
A program may use at most 128 MiB of HBM per device.

```python
import math
import jax
import jax.numpy as jnp
import numpy as np
from jax import lax

D = 2048
FF = 4096
MEMBERS = 4
TOP = 2
TOK_DEV = 128
BLOCK_FF = 1024
EXPERTS = 4
CAP = 80
TOKENS = 2048
N_EP = 16


def levels(stream_key, shape, shards, smallest, top_value):
    factor_of = 1.0
    for axis_at, blocks in shards:
        steps = jax.random.uniform(jax.random.fold_in(jax.random.fold_in(stream_key, 6), axis_at), (blocks,), jnp.float32, smallest / len(shards), top_value / len(shards))
        factor_of = factor_of * jnp.repeat(jnp.exp(steps), shape[axis_at] // blocks).reshape((-1,) + (1,) * (len(shape) - 1 - axis_at))
    return factor_of


def routed_block(stream_key, own, number, rows, count, top, most, lean):
    order = jax.random.permutation(stream_key, count)
    packed, common = shares(count, rows * top, most, lean, True), shares(count, rows * top, most, lean, False)
    places = jnp.arange(count)

    def named(sizes, rotation):
        used = int((sizes > 0).sum())
        fixed = max(1, used // 4)
        moved = fixed + (places - fixed + rotation * (used - fixed)) % max(1, count - fixed)
        return jnp.zeros((count,), jnp.int32).at[order[jnp.where(places < fixed, places, moved)]].set(jnp.asarray(sizes, jnp.int32))

    sizes = jnp.where(number % 4 == 0, named(packed, number // 4), named(common, number - number // 4 - 1))
    mixed = jax.random.permutation(jax.random.fold_in(own, 3), count)
    donor, taker = mixed[0:count // 2 * 2:2], mixed[1:count // 2 * 2:2]
    slack = jnp.minimum(sizes[donor] - 1, most - sizes[taker]) // 2
    slack = jnp.where((donor == order[0]) | (taker == order[0]) | (sizes[taker] == 0), 0, jnp.maximum(slack, 0))
    moved = jax.random.randint(jax.random.fold_in(own, 4), (count // 2,), 0, 1 << 20) % (slack + 1)
    sizes = sizes.at[donor].add(-moved).at[taker].add(moved)
    items = jnp.searchsorted(jnp.cumsum(sizes), jnp.arange(rows * top), side="right").astype(jnp.int32)
    table = items.reshape(top, rows).T
    table = table[jax.random.permutation(jax.random.fold_in(own, 1), rows)]
    rotation = jax.random.randint(jax.random.fold_in(own, 2), (rows, 1), 0, top)
    return jnp.take_along_axis(table, (jnp.arange(top)[None, :] + rotation) % top, axis=1)


def shares(number_of, total, limit, slope, full):
    loads = [(1 << 20) // math.isqrt(rank ** slope) + 1 for rank in range(1, number_of + 1)]
    largest = limit if full else min(limit, max(-(-total // number_of), total * loads[0] // sum(loads)))
    least = 1 if total - largest >= number_of - 1 else 0
    holding, surplus = [largest] + [least] * (number_of - 1), total - largest - least * (number_of - 1)
    while surplus > 0:
        free = [i for i in range(1, number_of) if holding[i] < largest] or [i for i in range(1, number_of) if holding[i] < limit]
        pool, budget = sum([loads[i] for i in free]), surplus
        for i in free:
            addition = min(limit - holding[i], max(1, budget * loads[i] // pool), surplus)
            holding[i] = holding[i] + addition
            surplus = surplus - addition
    return np.array(holding)


def scatter_about(stream_key, shape, width, limit, pieces=(), held_as=jnp.bfloat16):
    result = width * jax.random.normal(stream_key, shape, jnp.float32)
    if pieces:
        result = result * levels(stream_key, shape, pieces, -0.22, 0.18)
    return jnp.clip(result, -limit, limit).astype(held_as)


def setup_inputs(seed: int = 0) -> dict:
    key_list = jax.random.split(jax.random.key(seed), 8)
    tokens = scatter_about(key_list[0], (TOKENS, D), 1.0, 6.0, ((0, 16),))
    routes_keys = jax.random.split(jax.random.fold_in(key_list[1], 1), TOKENS // TOK_DEV)
    routes_turns = jax.random.permutation(jax.random.fold_in(key_list[1], 3), TOKENS // TOK_DEV)
    routes = jax.vmap(lambda own, number: routed_block(jax.random.fold_in(key_list[1], 2), own, number, TOK_DEV, EXPERTS, TOP, CAP, 2))(routes_keys, routes_turns).reshape((TOKENS, TOP))
    router_weight = scatter_about(key_list[2], (D, EXPERTS), D ** -0.5, 0.125)
    gate_proj = scatter_about(key_list[3], (EXPERTS * MEMBERS, D, BLOCK_FF), D ** -0.5, 0.125, ((0, 16), (2, 2)))
    up_proj = scatter_about(key_list[4], (EXPERTS * MEMBERS, D, BLOCK_FF), D ** -0.5, 0.125, ((0, 16), (2, 2)))
    down_proj = scatter_about(key_list[5], (EXPERTS * MEMBERS, BLOCK_FF, D), FF ** -0.5, 0.09375, ((0, 16), (1, 2)))
    cotangent = scatter_about(key_list[6], (TOKENS, D), 0.25, 1.5, ((0, 16),))
    return dict(tokens=tokens, routes=routes, router_weight=router_weight, gate_proj=gate_proj, up_proj=up_proj, down_proj=down_proj, cotangent=cotangent)


def expert_backward(tok_rows, cot_rows, gate_rows, w_gate, w_up, w_down):
    gpre = jnp.dot(tok_rows, w_gate, preferred_element_type=jnp.float32)
    upre = jnp.dot(tok_rows, w_up, preferred_element_type=jnp.float32)
    sig = jax.nn.sigmoid(gpre)
    silu_val = gpre * sig
    hidden = (silu_val * upre).astype(jnp.bfloat16)
    qvals = lax.dot_general(cot_rows, w_down, (((1,), (1,)), ((), ())), preferred_element_type=jnp.float32)
    gate_part = jnp.sum(hidden.astype(jnp.float32) * qvals, axis=1)
    weight = gate_rows[:, None]
    dhid = weight * qvals
    d_gate = (dhid * upre * sig * (1.0 + gpre * (1.0 - sig))).astype(jnp.bfloat16)
    d_up = (dhid * silu_val).astype(jnp.bfloat16)
    scaled = (weight * hidden.astype(jnp.float32)).astype(jnp.bfloat16)
    grad_down = lax.dot_general(scaled, cot_rows, (((0,), (0,)), ((), ())), preferred_element_type=jnp.float32)
    grad_gate = lax.dot_general(tok_rows, d_gate, (((0,), (0,)), ((), ())), preferred_element_type=jnp.float32)
    grad_up = lax.dot_general(tok_rows, d_up, (((0,), (0,)), ((), ())), preferred_element_type=jnp.float32)
    row_grad = lax.dot_general(d_gate, w_gate, (((1,), (1,)), ((), ())), preferred_element_type=jnp.float32)
    row_grad = row_grad + lax.dot_general(d_up, w_up, (((1,), (1,)), ((), ())), preferred_element_type=jnp.float32)
    return grad_gate, grad_up, grad_down, row_grad, gate_part


def reference(tokens, routes, router_weight, gate_proj, up_proj, down_proj, cotangent):
    ntok = tokens.shape[0]
    experts = router_weight.shape[1]
    slots = N_EP * CAP
    logits = jnp.dot(tokens, router_weight, preferred_element_type=jnp.float32)
    onehot = (routes[:, :, None] == jnp.arange(experts, dtype=jnp.int32)[None, None, :]).astype(jnp.float32)
    chosen = jnp.sum(onehot * logits[:, None, :], axis=2)
    first = jax.nn.sigmoid(chosen[:, 0] - chosen[:, 1])
    gates = jnp.stack([first, 1.0 - first], axis=1)
    used = lax.optimization_barrier(gates.astype(jnp.bfloat16)).astype(jnp.float32)
    flat = onehot.reshape(N_EP, TOK_DEV * TOP, experts)
    rank = jnp.cumsum(flat, axis=1) - flat
    rank_sel = jnp.sum(flat * rank, axis=2).reshape(ntok, TOP).astype(jnp.int32)
    source = (jnp.arange(ntok, dtype=jnp.int32) // TOK_DEV)[:, None]
    target = routes * slots + source * CAP + rank_sel
    token_ids = jnp.broadcast_to(jnp.arange(ntok, dtype=jnp.int32)[:, None], (ntok, TOP))
    slot_token = jnp.full((experts * slots,), ntok, jnp.int32).at[target.reshape(-1)].set(token_ids.reshape(-1))
    slot_gate = jnp.zeros((experts * slots,), jnp.float32).at[target.reshape(-1)].set(used.reshape(-1))
    slot_token = slot_token.reshape(experts, slots)
    slot_gate = slot_gate.reshape(experts, slots)
    zero_row = jnp.zeros((1, D), jnp.bfloat16)
    pad_tok = jnp.concatenate([tokens, zero_row], axis=0)
    pad_cot = jnp.concatenate([cotangent, zero_row], axis=0)
    full_gate = gate_proj.reshape(experts, MEMBERS, D, BLOCK_FF).transpose(0, 2, 1, 3).reshape(experts, D, FF)
    full_up = up_proj.reshape(experts, MEMBERS, D, BLOCK_FF).transpose(0, 2, 1, 3).reshape(experts, D, FF)
    full_down = down_proj.reshape(experts, FF, D)

    def one_expert(items):
        ids, gate_rows, w_gate, w_up, w_down = items
        return expert_backward(pad_tok[ids], pad_cot[ids], gate_rows, w_gate, w_up, w_down)

    grad_gate, grad_up, grad_down, row_grads, gate_parts = lax.map(
        one_expert, (slot_token, slot_gate, full_gate, full_up, full_down))
    route_sum = jax.ops.segment_sum(row_grads.reshape(-1, D), slot_token.reshape(-1), num_segments=ntok + 1)[:ntok]
    gate_grad = gate_parts.reshape(-1)[target]
    delta = first * (1.0 - first) * (gate_grad[:, 0] - gate_grad[:, 1])
    dlogits = delta[:, None] * (onehot[:, 0] - onehot[:, 1])
    router_part = jnp.dot(dlogits, router_weight.astype(jnp.float32).T, precision=lax.Precision.HIGHEST)
    token_grad = (route_sum + router_part).astype(jnp.bfloat16)
    router_grad = jnp.dot(tokens.astype(jnp.float32).T, dlogits, precision=lax.Precision.HIGHEST)
    gate_proj_grad = grad_gate.reshape(experts, D, MEMBERS, BLOCK_FF).transpose(0, 2, 1, 3).reshape(experts * MEMBERS, D, BLOCK_FF)
    up_proj_grad = grad_up.reshape(experts, D, MEMBERS, BLOCK_FF).transpose(0, 2, 1, 3).reshape(experts * MEMBERS, D, BLOCK_FF)
    down_proj_grad = grad_down.reshape(experts * MEMBERS, BLOCK_FF, D)
    return token_grad, gate_grad, router_grad, gate_proj_grad, up_proj_grad, down_proj_grad
```

```python
import jax
import jax.numpy as jnp
from jax import lax
from jax.sharding import PartitionSpec as P

MEMBERS = 4
TOP = 2
LANES = 128


def shards(tokens, routes, router_weight, gate_proj, up_proj, down_proj, cotangent):
    f32, bf16 = jnp.float32, jnp.bfloat16
    ntok, width = tokens.shape
    experts = router_weight.shape[1]
    n_ep = lax.axis_size("ep")
    n_tp = lax.axis_size("tp")
    share = width // n_tp
    cap = min(ntok, 5 * TOP * ntok // (4 * experts))
    lanes = -(-cap // LANES) * LANES
    tp = lax.axis_index("tp")
    ep = lax.axis_index("ep")
    mine = ep // MEMBERS
    member = ep % MEMBERS
    groups = [[0]]
    if experts > 1:
        groups.append(sorted({1, experts - 1}))
    if experts > 3:
        groups.append(list(range(2, experts - 1)))

    def flip(value, bit):
        return lax.ppermute(value, "ep", [(i, i ^ bit) for i in range(n_ep)])

    def shift(value, step):
        return lax.ppermute(
            value, "ep", [(i, (i + step * MEMBERS) % n_ep) for i in range(n_ep)]
        )

    def turn(value, step):
        return lax.ppermute(value, "tp", [(i, (i + step) % n_tp) for i in range(n_tp)])

    def direct(value, bit, step):
        return lax.ppermute(
            value,
            ("ep", "tp"),
            [
                (i * n_tp + j, (i ^ bit) * n_tp + (j + step) % n_tp)
                for i in range(n_ep)
                for j in range(n_tp)
            ],
        )

    def spread(value):
        return [value] + [turn(value, k) for k in range(1, n_tp)]

    def joined(pieces):
        columns = []
        for j in range(n_tp):
            piece = pieces[0]
            for k in range(1, n_tp):
                piece = jnp.where((tp - k) % n_tp == j, pieces[k], piece)
            columns.append(piece)
        return jnp.concatenate(columns, axis=1)

    onehot = (routes[:, :, None] == jnp.arange(experts, dtype=jnp.int32)[None, None, :]).astype(f32)
    flat = onehot.reshape(ntok * TOP, experts)
    order = jnp.arange(ntok * TOP, dtype=jnp.int32)
    before = (order[:, None] > order[None, :]).astype(bf16)
    rank = jnp.dot(before, flat.astype(bf16), preferred_element_type=f32)
    rank = jnp.sum(flat * rank, axis=1).astype(jnp.int32).reshape(ntok, TOP)
    slots = jnp.arange(experts * cap, dtype=jnp.int32)[:, None]
    away = (routes - mine) % experts * cap + rank
    place = ((slots == away[None, :, 0]) | (slots == away[None, :, 1])).astype(bf16)
    tok_part = lax.dynamic_slice_in_dim(tokens, tp * share, share, 1)
    cot_part = lax.dynamic_slice_in_dim(cotangent, tp * share, share, 1)
    tok_send = jnp.dot(place, tok_part, preferred_element_type=f32).astype(bf16)
    cot_send = jnp.dot(place, cot_part, preferred_element_type=f32).astype(bf16)

    logits = jnp.dot(tokens, router_weight, preferred_element_type=f32)
    chosen = jnp.sum(onehot * logits[:, None, :], axis=2)
    first = jax.nn.sigmoid(chosen[:, 0] - chosen[:, 1])
    gates = jnp.stack([first, 1.0 - first], axis=1)
    used = gates.astype(bf16).astype(f32)
    table = jnp.arange(lanes, dtype=jnp.int32)[None, None, :]
    hit = [
        (onehot[:, k, :].T[:, :, None] > 0) & (table == rank[:, k][None, :, None])
        for k in range(TOP)
    ]
    gate_slots = sum(
        jnp.sum(jnp.where(hit[k], used[None, :, k, None], 0.0), axis=1) for k in range(TOP)
    )
    gate_send = jnp.broadcast_to(
        gate_slots[:, None, None, :], (experts, MEMBERS, 1, lanes)
    ).reshape(n_ep, 1, lanes)
    gate_got = lax.all_to_all(gate_send, "ep", split_axis=0, concat_axis=0, tiled=True)
    gate_got = gate_got.reshape(n_ep, lanes)

    w_gate, w_up, w_down = gate_proj[0], up_proj[0], down_proj[0]

    def blocks_of(group):
        return [
            ((mine - d) % experts) * MEMBERS + jnp.bitwise_xor(member, 2 * i + j)
            for j in range(2)
            for i in range(2)
            for d in group
        ]

    tok_rows, cot_rows, dgs, dus, scs, parts, backs = [], [], [], [], [], [], {}
    arrived = {}
    for d in range(experts):
        block = slice(d * cap, (d + 1) * cap)
        if d == 0:
            arrived[d] = (tok_send[block], cot_send[block])
        else:
            arrived[d] = (shift(tok_send[block], d), shift(cot_send[block], d))

    sent = []
    for group in groups:
        tok = jnp.concatenate([arrived[d][0] for d in group], axis=0)
        cot = jnp.concatenate([arrived[d][1] for d in group], axis=0)
        tok_side = flip(tok, 2)
        cot_pieces = spread(cot)
        tok_near = joined(spread(tok))
        cot_far = joined([flip(piece, 2) for piece in cot_pieces])
        tok_far = joined(spread(tok_side))
        cot_near = joined(cot_pieces)
        tok_chip = jnp.concatenate([tok_near, tok_far], axis=0)
        cot_chip = jnp.concatenate([cot_near, cot_far], axis=0)
        sent.append((tok_chip, cot_chip, flip(tok_chip, 1), flip(cot_chip, 1)))

    for group, (tok_chip, cot_chip, tok_core, cot_core) in zip(groups, sent):
        half = tok_chip.shape[0]
        tok_all = jnp.concatenate([tok_chip, tok_core], axis=0)
        cot_all = jnp.concatenate([cot_chip, cot_core], axis=0)
        pick = (
            jnp.stack(blocks_of(group))[:, None] == jnp.arange(n_ep, dtype=jnp.int32)[None, :]
        ).astype(bf16)
        weight = jnp.dot(pick, gate_got.astype(bf16), preferred_element_type=f32)
        weight = weight[:, :cap].reshape(-1, 1)
        gpre = jnp.dot(tok_all, w_gate, preferred_element_type=f32)
        upre = jnp.dot(tok_all, w_up, preferred_element_type=f32)
        sig = jax.nn.sigmoid(gpre)
        silu_val = gpre * sig
        hidden = (silu_val * upre).astype(bf16)
        qvals = lax.dot_general(
            cot_all, w_down, (((1,), (1,)), ((), ())), preferred_element_type=f32
        )
        parts.append(jnp.sum(hidden.astype(f32) * qvals, axis=1))
        dhid = weight * qvals
        d_gate = (dhid * upre * sig * (1.0 + gpre * (1.0 - sig))).astype(bf16)
        d_up = (dhid * silu_val).astype(bf16)
        scaled = (weight * hidden.astype(f32)).astype(bf16)
        tok_rows.append(tok_all)
        cot_rows.append(cot_all)
        dgs.append(d_gate)
        dus.append(d_up)
        scs.append(scaled)
        row_grad = lax.dot_general(
            d_gate, w_gate, (((1,), (1,)), ((), ())), preferred_element_type=f32
        )
        row_grad = row_grad + lax.dot_general(
            d_up, w_up, (((1,), (1,)), ((), ())), preferred_element_type=f32
        )
        row_grad = row_grad.astype(bf16)
        summed = row_grad[:half].astype(f32) + flip(row_grad[half:], 1).astype(f32)
        summed = summed.astype(bf16)
        rows = half // 2
        total = None
        for i in range(2):
            for k in range(n_tp):
                value = lax.dynamic_slice(
                    summed, (i * rows, (tp + k) % n_tp * share), (rows, share)
                )
                if i or k:
                    value = direct(value, 2 * i, k)
                total = value.astype(f32) if total is None else total + value.astype(f32)
        total = total.astype(bf16)
        for at, d in enumerate(group):
            value = total[at * cap : (at + 1) * cap]
            backs[d] = value if d == 0 else shift(value, -d)

    flat_blocks = jnp.stack([b for group in groups for b in blocks_of(group)])
    part_table = jnp.concatenate(
        [part.reshape(-1, cap) for part in parts], axis=0
    )
    part_table = jnp.pad(part_table, ((0, 0), (0, lanes - cap)))
    pick = (jnp.arange(n_ep, dtype=jnp.int32)[:, None] == flat_blocks[None, :]).astype(f32)
    part_send = jnp.dot(pick, part_table, precision=lax.Precision.HIGHEST)
    part_got = lax.all_to_all(
        part_send.reshape(n_ep, 1, lanes), "ep", split_axis=0, concat_axis=0, tiled=True
    )
    part_got = jnp.sum(part_got.reshape(experts, MEMBERS, lanes), axis=1)
    back_gate = sum(turn(part_got, k) for k in range(1, n_tp)) + part_got if n_tp > 1 else part_got
    gate_grad = jnp.stack(
        [
            jnp.sum(jnp.where(hit[k], back_gate[:, None, :], 0.0), axis=(0, 2))
            for k in range(TOP)
        ],
        axis=1,
    )
    delta = first * (1.0 - first) * (gate_grad[:, 0] - gate_grad[:, 1])
    dlogits = delta[:, None] * (onehot[:, 0] - onehot[:, 1])
    router_part = lax.dot_general(
        dlogits, tokens.astype(f32), (((0,), (0,)), ((), ())), precision=lax.Precision.HIGHEST
    )
    router_send = router_part.reshape(experts, n_ep, width // n_ep).transpose(1, 0, 2)
    router_got = lax.all_to_all(router_send, "ep", split_axis=0, concat_axis=0, tiled=True)
    router_grad = jnp.sum(router_got, axis=0).T

    tok_rows, cot_rows = jnp.concatenate(tok_rows, axis=0), jnp.concatenate(cot_rows, axis=0)
    d_gate, d_up = jnp.concatenate(dgs, axis=0), jnp.concatenate(dus, axis=0)
    scaled = jnp.concatenate(scs, axis=0)
    across = (((0,), (0,)), ((), ()))
    grad_gate = lax.dot_general(tok_rows, d_gate, across, preferred_element_type=f32)
    grad_up = lax.dot_general(tok_rows, d_up, across, preferred_element_type=f32)
    grad_down = lax.dot_general(scaled, cot_rows, across, preferred_element_type=f32)

    back_rows = jnp.concatenate([backs[d] for d in range(experts)], axis=0)
    route_sum = lax.dot_general(place, back_rows, across, preferred_element_type=f32)
    router_rows = lax.dynamic_slice_in_dim(router_weight, tp * share, share, 0).astype(f32)
    from_router = lax.dot_general(
        dlogits, router_rows, (((1,), (1,)), ((), ())), precision=lax.Precision.HIGHEST
    )
    token_grad = (route_sum + from_router).astype(bf16)
    return (token_grad, gate_grad, router_grad, grad_gate[None], grad_up[None], grad_down[None])


def solution(mesh):
    placed = (
        P("ep", None),
        P("ep", None),
        P(),
        P("ep", None, "tp"),
        P("ep", None, "tp"),
        P("ep", "tp", None),
        P("ep", None),
    )
    return jax.shard_map(
        shards,
        mesh=mesh,
        in_specs=placed,
        out_specs=(
            P("ep", "tp"),
            P("ep", None),
            P("ep", None),
            P("ep", None, "tp"),
            P("ep", None, "tp"),
            P("ep", "tp", None),
        ),
        check_vma=False,
    )
```

```python
import functools

import jax
import jax.numpy as jnp
from jax import lax
from jax.experimental import pallas as pl
from jax.experimental.pallas import tpu as pltpu
from jax.sharding import PartitionSpec as P


MEMBERS = 4
TOP = 2
LANES = 128
TILE = 16
MIB = 1024 * 1024


f32, bf16, i32 = jnp.float32, jnp.bfloat16, jnp.int32
ACROSS = (((0,), (0,)), ((), ()))
BACK = (((1,), (1,)), ((), ()))
WHOLE = pl.BlockSpec(memory_space=pltpu.VMEM)
SCALARS = pl.BlockSpec(memory_space=pltpu.SMEM)


def mxu(a, b, dims=(((1,), (0,)), ((), ())), precision=None):
    return lax.dot_general(a, b, dims, preferred_element_type=f32, precision=precision)


def call(body, outs, args, limit=60, flops=0, moved=0, **kwargs):
    return pl.pallas_call(
        body,
        out_shape=outs,
        compiler_params=pltpu.CompilerParams(vmem_limit_bytes=limit * MIB),
        cost_estimate=pl.CostEstimate(
            flops=int(flops), bytes_accessed=int(moved), transcendentals=0
        ),
        **kwargs,
    )(*args)


def place_kernel(experts, cap, share, at_ref, routes_ref, tok_ref, cot_ref, place_ref, *outs):
    mine, start = at_ref[0], pl.multiple_of(at_ref[1] * share, LANES)
    ntok = routes_ref.shape[1]
    tall = -(-experts // TILE) * TILE
    kind = lax.broadcasted_iota(i32, (tall, ntok), 0)
    named = jnp.zeros((tall, ntok), f32)
    for k in range(TOP):
        away = routes_ref[k : k + 1, :] - mine
        away = jnp.where(away < 0, away + experts, away)
        named = named + jnp.where(kind == away, 1.0, 0.0)
    row = lax.broadcasted_iota(i32, (ntok, ntok), 0)
    column = lax.broadcasted_iota(i32, (ntok, ntok), 1)
    rank = mxu(named.astype(bf16), jnp.where(row < column, 1.0, 0.0).astype(bf16))
    rank = jnp.where(named > 0.5, rank, -1.0)
    slot = lax.broadcasted_iota(i32, (cap, ntok), 0).astype(f32)
    tok = tok_ref[:, pl.ds(start, share)]
    cot = cot_ref[:, pl.ds(start, share)]
    for d in range(experts):
        place = jnp.where(slot == rank[d : d + 1], 1.0, 0.0).astype(bf16)
        place_ref[d] = place
        outs[d][...] = mxu(place, tok).astype(bf16)
        outs[experts + d][...] = mxu(place, cot).astype(bf16)


def terms(value):
    parts = []
    for _ in range(3):
        parts.append(value.astype(bf16))
        value = value - parts[-1].astype(f32)
    return parts


def gates_kernel(experts, cap, at_ref, routes_ref, tok_ref, router_ref, place_ref, first_ref, *outs):
    logits = mxu(router_ref[...], tok_ref[...], BACK)
    ntok, lanes = logits.shape[1], outs[0].shape[1]
    kind = lax.broadcasted_iota(i32, (experts, ntok), 0)
    chosen = [
        jnp.sum(jnp.where(kind == routes_ref[k : k + 1, :], logits, 0.0), axis=0, keepdims=True)
        for k in range(TOP)
    ]
    first = jax.nn.sigmoid(chosen[0] - chosen[1])
    first_ref[...] = first
    used = [first.astype(bf16).astype(f32), (1.0 - first).astype(bf16).astype(f32)]
    for d in range(experts):
        value = jnp.zeros((1, ntok), f32)
        for k in range(TOP):
            away = routes_ref[k : k + 1, :] - at_ref[0]
            away = jnp.where(away < 0, away + experts, away)
            value = value + jnp.where(away == d, used[k], 0.0)
        value = jnp.broadcast_to(value, (8, ntok)).astype(bf16)
        slots = mxu(value, place_ref[d], BACK)[:1]
        outs[d][...] = jnp.zeros((1, lanes), f32)
        outs[d][:, :cap] = slots


def expert_kernel(
    layout, n_tp, share, tp_ref, tok_ref, cot_ref, gate_ref, wg_ref, wu_ref, wd_ref,
    dg_ref, du_ref, sc_ref, rg_ref, part_ref,
):
    group, experts, cap = layout
    rows, lanes = tok_ref.shape[0], gate_ref.shape[1]
    step = pl.program_id(0)
    starts = [
        pl.multiple_of(lax.rem(tp_ref[0] - k + n_tp, n_tp) * share, LANES) for k in range(n_tp)
    ]
    spans = [slice(k * share, (k + 1) * share) for k in range(n_tp)]
    gpre = sum(mxu(tok_ref[:, s], wg_ref[pl.ds(a, share), :]) for s, a in zip(spans, starts))
    upre = sum(mxu(tok_ref[:, s], wu_ref[pl.ds(a, share), :]) for s, a in zip(spans, starts))
    qvals = sum(
        mxu(cot_ref[:, s], wd_ref[:, pl.ds(a, share)], BACK) for s, a in zip(spans, starts)
    )

    entry = lax.broadcasted_iota(i32, (1, 2 * experts), 1)
    low = jnp.full((1, 2 * experts), -cap, i32)
    for i in range(2):
        for at, d in enumerate(group):
            low = jnp.where(entry == i * experts + d, (i * len(group) + at) * cap, low)
    row = lax.broadcasted_iota(i32, (rows, 1), 0) + step * rows
    mine = (row >= low) & (row < low + cap)
    slot = row - jnp.sum(jnp.where(mine, low, 0), axis=1, keepdims=True)
    mine = jnp.where(mine, 1.0, 0.0)
    seat = lax.broadcasted_iota(i32, (rows, lanes), 1) == slot
    weight = mxu(mine.astype(bf16), gate_ref[...].astype(bf16))
    weight = jnp.sum(jnp.where(seat, weight, 0.0), axis=1, keepdims=True)

    sig = jax.nn.sigmoid(gpre)
    silu_val = gpre * sig
    hidden = (silu_val * upre).astype(bf16)
    wide = hidden.astype(f32)
    part = jnp.sum(wide * qvals, axis=1, keepdims=True)
    ones = mine.astype(bf16)
    part = sum(mxu(ones, term, ACROSS) for term in terms(jnp.where(seat, part, 0.0)))

    @pl.when(step == 0)
    def _():
        part_ref[...] = part

    @pl.when(step > 0)
    def _():
        part_ref[...] += part

    dhid = weight * qvals
    d_gate = (dhid * upre * sig * (1.0 + gpre * (1.0 - sig))).astype(bf16)
    d_up = (dhid * silu_val).astype(bf16)
    dg_ref[...] = d_gate
    du_ref[...] = d_up
    sc_ref[...] = (weight * wide).astype(bf16)
    for s, a in zip(spans, starts):
        total = mxu(d_gate, wg_ref[pl.ds(a, share), :], BACK)
        total = total + mxu(d_up, wu_ref[pl.ds(a, share), :], BACK)
        rg_ref[:, s] = total.astype(bf16)


def parts_kernel(experts, n, at_ref, *refs):
    out = refs[2 * n]
    mine, member = at_ref[0], at_ref[2]
    n_ep, lanes = out.shape[0], out.shape[2]
    entry = lax.broadcasted_iota(i32, (1, 2 * experts), 1)
    i = jnp.where(entry >= experts, 1, 0)
    away = mine - (entry - i * experts)
    away = jnp.where(away < 0, away + experts, away)
    device = lax.broadcasted_iota(i32, (n_ep, 2 * experts), 0)
    total = jnp.zeros((n_ep, lanes), f32)
    for j in range(2):
        table = refs[j * n][...]
        for c in range(1, n):
            table = table + refs[j * n + c][...]
        owner = away * MEMBERS + jnp.bitwise_xor(member, 2 * i + j)
        pick = jnp.where(device == owner, 1.0, 0.0).astype(bf16)
        total = total + sum(mxu(pick, term) for term in terms(table))
    for e in range(n_ep):
        out[e] = total[e : e + 1, :]


def router_kernel(
    experts, cap, n, at_ref, routes_ref, tok_ref, place_ref, first_ref, *refs
):
    gate_ref, change_ref, out_ref = refs[n:]
    ntok = routes_ref.shape[1]
    values = []
    for d in range(experts):
        source = lax.rem(at_ref[0] + d, experts)
        back = refs[0][pl.ds(source, 1), :]
        for ref in refs[1:n]:
            back = back + ref[pl.ds(source, 1), :]
        back = jnp.broadcast_to(back[:, :cap], (8, cap))
        values.append(sum(mxu(term, place_ref[d]) for term in terms(back))[:1])
    grads = []
    for k in range(TOP):
        away = routes_ref[k : k + 1, :] - at_ref[0]
        away = jnp.where(away < 0, away + experts, away)
        value = jnp.zeros((1, ntok), f32)
        for d in range(experts):
            value = value + jnp.where(away == d, values[d], 0.0)
        gate_ref[k : k + 1, :] = value
        grads.append(value)
    first = first_ref[...]
    delta = first * (1.0 - first) * (grads[0] - grads[1])
    kind = lax.broadcasted_iota(i32, (experts, ntok), 0)
    change = jnp.where(kind == routes_ref[0:1, :], delta, 0.0)
    change = change - jnp.where(kind == routes_ref[1:2, :], delta, 0.0)
    change_ref[...] = change
    total = sum(mxu(term, tok_ref[...]) for term in terms(change))
    n_ep, span = out_ref.shape[0], out_ref.shape[2]
    for e in range(n_ep):
        out_ref[e] = total[:, e * span : (e + 1) * span]


def pair_kernel(counts, n_tp, share, *refs):
    n = len(counts)
    outs = refs[2 * n :]
    low = 0
    for c, rows in enumerate(counts):
        for i in range(2):
            for k in range(n_tp):
                piece = (slice(i * rows, (i + 1) * rows), slice(k * share, (k + 1) * share))
                total = refs[2 * c][piece].astype(f32) + refs[2 * c + 1][piece].astype(f32)
                outs[i * n_tp + k][low : low + rows, :] = total.astype(bf16)
        low += rows


def total_kernel(n, cap, *refs):
    outs = refs[n:]
    for at, out in enumerate(outs):
        piece = slice(at * cap, (at + 1) * cap)
        total = refs[0][piece, :].astype(f32)
        for ref in refs[1:n]:
            total = total + ref[piece, :].astype(f32)
        out[...] = total.astype(bf16)


def token_kernel(experts, share, at_ref, place_ref, change_ref, router_ref, *refs):
    start = pl.multiple_of(at_ref[1] * share, LANES)
    router = router_ref[:, pl.ds(start, share)]
    total = sum(mxu(term, router, ACROSS) for term in terms(change_ref[...]))
    for d in range(experts):
        total = total + mxu(place_ref[d], refs[d][...], ACROSS)
    refs[experts][...] = total.astype(bf16)


def in_grads_kernel(n, tp_ref, *refs):
    gate_ref, up_ref, tok_all, gates, ups = refs[3 * n :]

    def gather(refs, target):
        low = 0
        for ref in refs:
            target[low : low + ref.shape[0], :] = ref[...]
            low += ref.shape[0]

    @pl.when(pl.program_id(0) == 0)
    def _():
        gather(refs[n : 2 * n], gates)
        gather(refs[2 * n : 3 * n], ups)

    gather(refs[:n], tok_all)
    flipped = tok_all[...].T
    gate_ref[...] = mxu(flipped, gates[...])
    up_ref[...] = mxu(flipped, ups[...])


def out_grad_kernel(n, tp_ref, *refs):
    down_ref, cot_all, scaled = refs[2 * n :]
    low = 0
    for ref in refs[:n]:
        cot_all[low : low + ref.shape[0], :] = ref[...]
        low += ref.shape[0]

    @pl.when(pl.program_id(0) == 0)
    def _():
        low = 0
        for ref in refs[n : 2 * n]:
            scaled[:, low : low + ref.shape[0]] = ref[...].T
            low += ref.shape[0]

    down_ref[...] = mxu(scaled[...], cot_all[...])


def grouped(experts):
    near = sorted({0, 1 % experts, (experts - 1) % experts})
    rest = [d for d in range(experts) if d not in near]
    return [near] + ([rest] if rest else [])


def shards(tokens, routes, router_weight, gate_proj, up_proj, down_proj, cotangent):
    ntok, width = tokens.shape
    experts = router_weight.shape[1]
    n_ep = lax.axis_size("ep")
    n_tp = lax.axis_size("tp")
    share = width // n_tp
    hidden_units = gate_proj.shape[2]
    cap = min(ntok, 5 * TOP * ntok // (4 * experts))
    cap = -(-cap // TILE) * TILE
    lanes = -(-cap // LANES) * LANES
    tp = lax.axis_index("tp")
    ep = lax.axis_index("ep")
    mine = ep // MEMBERS
    member = ep % MEMBERS
    groups = grouped(experts)
    shape = jax.ShapeDtypeStruct

    def flip(value, bit):
        return lax.ppermute(value, "ep", [(i, i ^ bit) for i in range(n_ep)])

    def shift(value, step):
        pairs = [(i, (i + step * MEMBERS) % n_ep) for i in range(n_ep)]
        return lax.ppermute(value, "ep", pairs)

    def turn(value, step):
        return lax.ppermute(value, "tp", [(i, (i + step) % n_tp) for i in range(n_tp)])

    def direct(value, bit, step):
        pairs = [
            (i * n_tp + j, (i ^ bit) * n_tp + (j + step) % n_tp)
            for i in range(n_ep)
            for j in range(n_tp)
        ]
        return lax.ppermute(value, ("ep", "tp"), pairs)

    def spread(value):
        return [value] + [turn(value, k) for k in range(1, n_tp)]

    at = jnp.stack([mine, tp, member]).astype(i32)
    router = router_weight.T

    placed = call(
        functools.partial(place_kernel, experts, cap, share),
        [shape((experts, cap, ntok), bf16)] + [shape((cap, share), bf16)] * (2 * experts),
        (at, routes.T, tokens, cotangent),
        in_specs=[SCALARS] + [WHOLE] * 3,
        out_specs=[WHOLE] * (1 + 2 * experts),
        flops=4 * experts * cap * ntok * share,
        moved=4 * ntok * width,
    )
    place, tok_send, cot_send = placed[0], placed[1 : 1 + experts], placed[1 + experts :]
    arrived = {0: (tok_send[0], cot_send[0])}
    for d in range(1, experts):
        arrived[d] = (shift(tok_send[d], d), shift(cot_send[d], d))

    first, *gate_slots = call(
        functools.partial(gates_kernel, experts, cap),
        [shape((1, ntok), f32)] + [shape((1, lanes), f32)] * experts,
        (at, routes.T, tokens, router, place),
        in_specs=[SCALARS] + [WHOLE] * 4,
        out_specs=[WHOLE] * (1 + experts),
        flops=4 * ntok * width * LANES,
        moved=2 * ntok * width,
    )
    gate_rows = jnp.concatenate(
        gate_slots[:1] + [shift(gate_slots[d], d) for d in range(1, experts)], axis=0
    )
    gate_chip = jnp.concatenate([gate_rows, flip(gate_rows, 2)], axis=0)
    gate_tables = (gate_chip, flip(gate_chip, 1))

    sent = []
    for group in groups:
        tok, cot = arrived[group[0]]
        if len(group) > 1:
            tok = jnp.concatenate([arrived[d][0] for d in group], axis=0)
            cot = jnp.concatenate([arrived[d][1] for d in group], axis=0)
        tok_near, cot_near = spread(tok), spread(cot)
        tok_far = spread(flip(tok, 2))
        cot_far = [flip(piece, 2) for piece in cot_near]
        tok_chip = jnp.concatenate(
            [jnp.concatenate(tok_near, axis=1), jnp.concatenate(tok_far, axis=1)], axis=0
        )
        cot_chip = jnp.concatenate(
            [jnp.concatenate(cot_near, axis=1), jnp.concatenate(cot_far, axis=1)], axis=0
        )
        sent.append(((tok_chip, cot_chip), (flip(tok_chip, 1), flip(cot_chip, 1))))

    w_gate, w_up, w_down = gate_proj[0], up_proj[0], down_proj[0]
    at_tp = tp.astype(i32).reshape(1)

    def experts_on(group, rows_of, gate_table):
        tok, cot = rows_of
        rows = tok.shape[0]
        block = rows if rows <= 512 else rows // 2
        across = lambda s, tp_ref: (s, 0)
        still = lambda s, tp_ref: (0, 0)
        wide = pl.BlockSpec((block, width), across)
        narrow = pl.BlockSpec((block, hidden_units), across)
        return call(
            functools.partial(expert_kernel, (group, experts, cap), n_tp, share),
            [shape((rows, hidden_units), bf16)] * 3
            + [shape((rows, width), bf16), shape((2 * experts, lanes), f32)],
            (at_tp, tok, cot, gate_table, w_gate, w_up, w_down),
            limit=36,
            flops=10 * rows * width * hidden_units,
            moved=6 * rows * width + 6 * width * hidden_units,
            grid_spec=pltpu.PrefetchScalarGridSpec(
                num_scalar_prefetch=1,
                grid=(rows // block,),
                in_specs=[wide, wide, pl.BlockSpec((2 * experts, lanes), still)]
                + [pl.BlockSpec((width, hidden_units), still)] * 2
                + [pl.BlockSpec((hidden_units, width), still)],
                out_specs=[narrow] * 3 + [wide, pl.BlockSpec((2 * experts, lanes), still)],
            ),
        )

    toks, cots, dgs, dus, scs, parts, grads = [], [], [], [], [], ([], []), []
    for group, pair in zip(groups, sent):
        here = []
        for j in range(2):
            dg, du, sc, rg, part = experts_on(group, pair[j], gate_tables[j])
            toks.append(pair[j][0])
            cots.append(pair[j][1])
            dgs.append(dg)
            dus.append(du)
            scs.append(sc)
            parts[j].append(part)
            here.append(rg)
        grads.append((here[0], flip(here[1], 1)))

    backs = {}
    last = len(groups) - 1
    for chunk in [[c] for c in range(last + 1)]:
        members = [d for c in chunk for d in groups[c]]
        counts = [len(groups[c]) * cap for c in chunk]
        rows = sum(counts)
        pieces = call(
            functools.partial(pair_kernel, counts, n_tp, share),
            [shape((rows, share), bf16)] * (2 * n_tp),
            [value for c in chunk for value in grads[c]],
            in_specs=[WHOLE] * (2 * len(chunk)),
            out_specs=[WHOLE] * (2 * n_tp),
            flops=2 * rows * width,
            moved=12 * rows * width,
        )
        pieces = [
            direct(pieces[i * n_tp + k], 2 * i, -k) if i or k else pieces[0]
            for i in range(2)
            for k in range(n_tp)
        ]
        totals = call(
            functools.partial(total_kernel, 2 * n_tp, cap),
            [shape((cap, share), bf16)] * len(members),
            pieces,
            in_specs=[WHOLE] * (2 * n_tp),
            out_specs=[WHOLE] * len(members),
            limit=24,
            flops=2 * rows * width,
            moved=6 * rows * width,
        )
        for d, value in zip(members, totals):
            backs[d] = shift(value, -d) if d else value

    part_send = call(
        functools.partial(parts_kernel, experts, len(groups)),
        shape((n_ep, 1, lanes), f32),
        (at, *parts[0], *parts[1]),
        in_specs=[SCALARS] + [WHOLE] * (2 * len(groups)),
        out_specs=WHOLE,
        flops=6 * n_ep * experts * lanes,
    )
    part_got = lax.all_to_all(part_send, "ep", split_axis=0, concat_axis=0, tiled=True)
    part_got = jnp.sum(part_got.reshape(experts, MEMBERS, lanes), axis=1)
    gate_back = [part_got] + [turn(part_got, k) for k in range(1, n_tp)]
    gate_grad, change, router_send = call(
        functools.partial(router_kernel, experts, cap, n_tp),
        [
            shape((TOP, ntok), f32),
            shape((experts, ntok), f32),
            shape((n_ep, experts, width // n_ep), f32),
        ],
        (at, routes.T, tokens, place, first, *gate_back),
        in_specs=[SCALARS] + [WHOLE] * (4 + n_tp),
        out_specs=[WHOLE] * 3,
        flops=6 * ntok * width * LANES,
        moved=2 * ntok * width,
    )
    router_got = lax.all_to_all(router_send, "ep", split_axis=0, concat_axis=0, tiled=True)
    router_grad = jnp.sum(router_got, axis=0).T

    n = len(toks)
    block = min(share, 512)
    per = share // block

    def home(s, tp_ref):
        return lax.rem(tp_ref[0] - s // per + n_tp, n_tp) * per + s % per

    step_of = lambda s, tp_ref: (0, s)
    still = lambda s, tp_ref: (0, 0)
    rows = sum(v.shape[0] for v in toks)
    grad_gate, grad_up = call(
        functools.partial(in_grads_kernel, n),
        [shape((width, hidden_units), f32)] * 2,
        (at_tp, *toks, *dgs, *dus),
        flops=4 * rows * width * hidden_units,
        moved=2 * rows * width + 8 * width * hidden_units,
        grid_spec=pltpu.PrefetchScalarGridSpec(
            num_scalar_prefetch=1,
            grid=(width // block,),
            in_specs=[pl.BlockSpec((v.shape[0], block), step_of) for v in toks]
            + [pl.BlockSpec(v.shape, still) for v in dgs + dus],
            out_specs=[
                pl.BlockSpec((block, hidden_units), lambda s, tp_ref: (home(s, tp_ref), 0))
            ]
            * 2,
            scratch_shapes=[pltpu.VMEM((rows, block), bf16)]
            + [pltpu.VMEM((rows, hidden_units), bf16)] * 2,
        ),
    )
    grad_down = call(
        functools.partial(out_grad_kernel, n),
        shape((hidden_units, width), f32),
        (at_tp, *cots, *scs),
        flops=2 * rows * width * hidden_units,
        moved=2 * rows * width + 4 * width * hidden_units,
        grid_spec=pltpu.PrefetchScalarGridSpec(
            num_scalar_prefetch=1,
            grid=(width // block,),
            in_specs=[pl.BlockSpec((v.shape[0], block), step_of) for v in cots]
            + [pl.BlockSpec(v.shape, still) for v in scs],
            out_specs=pl.BlockSpec((hidden_units, block), lambda s, tp_ref: (0, home(s, tp_ref))),
            scratch_shapes=[
                pltpu.VMEM((rows, block), bf16),
                pltpu.VMEM((hidden_units, rows), bf16),
            ],
        ),
    )

    token_grad = call(
        functools.partial(token_kernel, experts, share),
        shape((ntok, share), bf16),
        (at, place, change, router, *[backs[d] for d in range(experts)]),
        in_specs=[SCALARS] + [WHOLE] * (3 + experts),
        out_specs=WHOLE,
        limit=24,
        flops=2 * experts * cap * ntok * share,
        moved=6 * experts * cap * share,
    )
    return (
        token_grad, gate_grad.T, router_grad, grad_gate[None], grad_up[None], grad_down[None]
    )


def solution(mesh):
    placed = (
        P("ep", None),
        P("ep", None),
        P(),
        P("ep", None, "tp"),
        P("ep", None, "tp"),
        P("ep", "tp", None),
        P("ep", None),
    )

    return jax.shard_map(
        shards,
        mesh=mesh,
        in_specs=placed,
        out_specs=(
            P("ep", "tp"),
            P("ep", None),
            P("ep", None),
            P("ep", None, "tp"),
            P("ep", None, "tp"),
            P("ep", "tp", None),
        ),
        check_vma=False,
    )
```
